32 devices in a mesh: sp: 8 (over z, x), dp: 4 (over y, core).
Axes of the slice: x: 2, y: 2, z: 4, core: 2. Of those that a mesh axis runs over, the one named last changes fastest.
Arguments:
- residual_in: bfloat16 [4, 1024, 2048], P('dp', 'sp'), may hold values from -6 to 6
- query_proj: bfloat16 [4, 1024, 2048], P('dp', 'sp'), may hold values from -8 to 8
- key_proj: bfloat16 [4, 1024, 512], P('dp', 'sp'), may hold values from -8 to 8
- value_proj: bfloat16 [4, 1024, 512], P('dp', 'sp'), may hold values from -6 to 6
- query_gain: float32 [128], replicated, may hold values from 0.1 to 7
- key_gain: float32 [128], replicated, may hold values from 0.1 to 7
- out_weight: bfloat16 [2048, 2048], replicated, may hold values from -0.125 to 0.125
- post_gain: float32 [2048], replicated, may hold values from 0.1 to 1.9
- pre_gain: float32 [2048], replicated, may hold values from 0.1 to 1.9
- route_ids: int32 [4, 1024, 2], P('dp', 'sp'), may hold values from 0 to 31, as said below
- group_weight: float32 [4, 1024], P('dp', 'sp'), may hold values from 0.25 to 1
- first_share: float32 [4, 1024], P('dp', 'sp'), may hold values from 0.5 to 1
- gate_weight: bfloat16 [32, 2048, 512], P(('sp', 'dp')), may hold values from -0.125 to 0.125
- up_weight: bfloat16 [32, 2048, 512], P(('sp', 'dp')), may hold values from -0.125 to 0.125
- down_weight: bfloat16 [32, 512, 2048], P(('sp', 'dp')), may hold values from -0.25 to 0.25
Outputs:
- layer_out: bfloat16 [4, 1024, 2048], P('dp', 'sp')
The draws below stay inside these ranges and needn't reach their ends.
Inputs may be any that keep to these rules, and one draw needn't show every extreme that they name: `route_ids`: each token names two different experts of one group of 8 consecutive experts. Among the 128 tokens of one device each group is chosen by exactly 32 tokens, no expert is named by more than 16 of them, and in every draw one expert of each group is named by exactly 16 tokens of every device.
All inputs are finite; a program needn't handle non-finite values.
Results may differ from the reference program's by a relative error of at most 0.009.
The reference program's roundings to bfloat16 on the way count: a program that leaves them out, or rounds other values in their place, can miss the bound.
Values may be sent and summed in bfloat16 or wider, within the bound.
A program may use at most 128 MiB of HBM per device.

```python
import jax
import jax.numpy as jnp
from jax import lax

D = 2048
HEADS = 16
KV_HEADS = 4
HEAD_DIM = 128
FF = 512
GROUPS = 4
GRID_W = 64
TOK_DEV = 128
SEQS = 4
SEQ = 1024
EXPERTS = 32
CAP = 16
N_SP = 8
N_DP = 4


def draw_query_proj(key, part):
    own = jax.random.fold_in(key, 11)
    base = jax.random.truncated_normal(own, -6.0, 6.0, (SEQS, SEQ, HEADS * HEAD_DIM), jnp.float32)
    return base.astype(jnp.bfloat16)


def draw_key_proj(key, part):
    own = jax.random.fold_in(key, 12)
    base = jax.random.truncated_normal(own, -6.0, 6.0, (SEQS, SEQ, KV_HEADS * HEAD_DIM), jnp.float32)
    return base.astype(jnp.bfloat16)


def gain_table(own):
    return 1.0 + 0.18 * jax.random.truncated_normal(own, -5.0, 5.0, (HEAD_DIM,), jnp.float32)


def draw_query_gain(key, part):
    return gain_table(jax.random.fold_in(key, 21))


def draw_key_gain(key, part):
    return gain_table(jax.random.fold_in(key, 22))


def draw_route_ids(key, part):
    per_group = TOK_DEV // GROUPS
    group_width = EXPERTS // GROUPS
    middle = CAP // 2
    hot = jax.random.randint(jax.random.fold_in(key, 31), (GROUPS,), 0, group_width)
    block_count = SEQS * (SEQ // TOK_DEV)

    def one_block(block_key):
        key_tok, key_rest = jax.random.split(block_key)
        order = jax.random.permutation(key_tok, TOK_DEV)
        firsts = []
        seconds = []
        for group_id in range(GROUPS):
            group_key = jax.random.fold_in(key_rest, group_id)
            key_perm, key_shift, key_swap = jax.random.split(group_key, 3)
            shuffled = jax.random.permutation(key_perm, group_width).astype(jnp.int32)
            shifts = jax.random.randint(key_shift, (group_width // 2,), -middle, middle + 1)
            hot_place = jnp.sum(jnp.where(shuffled == hot[group_id], jnp.arange(group_width, dtype=jnp.int32), 0))
            sign_value = 1 - 2 * (hot_place % 2)
            shifts = shifts.at[hot_place // 2].set(middle * sign_value)
            counts = jnp.zeros((group_width,), jnp.int32).at[shuffled[0::2]].set(middle + shifts).at[shuffled[1::2]].set(middle - shifts)
            listed = jnp.repeat(jnp.arange(group_width, dtype=jnp.int32), counts, total_repeat_length=2 * per_group)
            first_pick = listed[:per_group]
            second_pick = listed[per_group:]
            swap_bits = jax.random.randint(key_swap, (per_group,), 0, 2)
            leading = jnp.where(swap_bits == 1, second_pick, first_pick)
            trailing = jnp.where(swap_bits == 1, first_pick, second_pick)
            firsts.append(leading + group_id * group_width)
            seconds.append(trailing + group_id * group_width)
        pairs = jnp.stack([jnp.concatenate(firsts), jnp.concatenate(seconds)], axis=1).astype(jnp.int32)
        return jnp.zeros((TOK_DEV, 2), jnp.int32).at[order].set(pairs)
    blocks_all = jax.vmap(one_block)(jax.random.split(jax.random.fold_in(key, 32), block_count))
    return blocks_all.reshape(SEQS, SEQ, 2)


def level_of(rng, shape, cuts, least, top_value):
    level, own = 1.0, jax.random.fold_in(rng, 6)
    for axis_at, shards_of in cuts:
        steps = jnp.exp(jax.random.uniform(jax.random.fold_in(own, axis_at), (shards_of,), jnp.float32, least / len(cuts), top_value / len(cuts)))
        level = level * jnp.repeat(steps, shape[axis_at] // shards_of).reshape([-1 if axis == axis_at else 1 for axis in range(len(shape))])
    return level


def bell_draw(key, shape, deviation, bound, cuts=(), kind=jnp.bfloat16):
    entries = jax.random.normal(key, shape, jnp.float32) * deviation
    if len(cuts) > 0:
        entries = level_of(key, shape, cuts, -0.22, 0.18) * entries
    return jnp.clip(entries, min=-bound, max=bound).astype(kind)


def setup_inputs(seed: int = 0) -> dict:
    keys = jax.random.split(jax.random.key(seed), 16)
    residual_in = bell_draw(keys[0], (SEQS, SEQ, D), 1.0, 6.0, ((0, 4), (1, 8)))
    query_proj = draw_query_proj(jax.random.fold_in(keys[15], 71), 0)
    key_proj = draw_key_proj(jax.random.fold_in(keys[15], 71), 0)
    value_proj = bell_draw(keys[3], (SEQS, SEQ, KV_HEADS * HEAD_DIM), 1.0, 6.0, ((0, 4), (1, 8)))
    query_gain = draw_query_gain(jax.random.fold_in(keys[15], 71), 0)
    key_gain = draw_key_gain(jax.random.fold_in(keys[15], 71), 0)
    out_weight = bell_draw(keys[6], (D, D), D ** -0.5, 0.125)
    post_gain = jnp.clip(1.0 + 0.18 * jax.random.normal(keys[7], (D,), jnp.float32), 0.1, 1.9)
    pre_gain = jnp.clip(1.0 + 0.18 * jax.random.normal(keys[8], (D,), jnp.float32), 0.1, 1.9)
    route_ids = draw_route_ids(jax.random.fold_in(keys[15], 71), 0)
    group_weight = jnp.clip(0.25 + 0.75 * jax.random.uniform(keys[10], (SEQS, SEQ), jnp.float32) ** level_of(keys[10], (SEQS, SEQ), ((0, 4), (1, 8)), -0.2, 0.2), 0.25, 1.0)
    first_share = jnp.clip(0.5 + 0.5 * jax.random.uniform(keys[11], (SEQS, SEQ), jnp.float32) ** level_of(keys[11], (SEQS, SEQ), ((0, 4), (1, 8)), -0.2, 0.2), 0.5, 1.0)
    gate_weight = bell_draw(keys[12], (EXPERTS, D, FF), D ** -0.5, 0.125, ((0, 32),))
    up_weight = bell_draw(keys[13], (EXPERTS, D, FF), D ** -0.5, 0.125, ((0, 32),))
    down_weight = bell_draw(keys[14], (EXPERTS, FF, D), FF ** -0.5, 0.25, ((0, 32),))
    return {"residual_in": residual_in, "query_proj": query_proj, "key_proj": key_proj, "value_proj": value_proj, "query_gain": query_gain, "key_gain": key_gain, "out_weight": out_weight, "post_gain": post_gain, "pre_gain": pre_gain, "route_ids": route_ids, "group_weight": group_weight, "first_share": first_share, "gate_weight": gate_weight, "up_weight": up_weight, "down_weight": down_weight}


EPSILON = 1e-06

def rotate_heads(raw_heads, gain_vec, positions):
    floats = raw_heads.astype(jnp.float32)
    normed = floats * lax.rsqrt(lax.optimization_barrier(jnp.mean(floats * floats, axis=-1, keepdims=True)) + EPSILON) * gain_vec
    quarter = raw_heads.shape[-1] // 4
    inverse = 10000.0 ** (-jnp.arange(quarter, dtype=jnp.float32) / quarter)
    grid_rows = (positions // GRID_W).astype(jnp.float32)[:, None] * inverse
    grid_cols = (positions % GRID_W).astype(jnp.float32)[:, None] * inverse
    angles = jnp.concatenate([grid_rows, grid_rows, grid_cols, grid_cols], axis=-1)[:, None, :]
    pieces = normed.reshape(normed.shape[:-1] + (2, 2, quarter))
    turned = jnp.stack([-pieces[..., 1, :], pieces[..., 0, :]], axis=-2).reshape(normed.shape)
    return (normed * jnp.cos(angles) + turned * jnp.sin(angles)).astype(jnp.bfloat16)

def attend_blocks(queries, keys_all, values_all):
    count_q, kv_count, group_size, head_width = queries.shape
    block = min(512, count_q)
    blocks = count_q // block
    scale = head_width ** (-0.5)
    zero_index = jnp.zeros((), jnp.int32)

    def one_item(item):
        which = (item // kv_count).astype(jnp.int32)
        head_index = (item % kv_count).astype(jnp.int32)
        start_row = (which * block).astype(jnp.int32)
        q_block = lax.dynamic_slice(queries, (start_row, head_index, zero_index, zero_index), (block, 1, group_size, head_width))[:, 0]
        key_block = lax.dynamic_slice(keys_all, (zero_index, head_index, zero_index), (keys_all.shape[0], 1, head_width))[:, 0]
        value_block = lax.dynamic_slice(values_all, (zero_index, head_index, zero_index), (values_all.shape[0], 1, head_width))[:, 0]
        scores = jnp.einsum('qgd,sd->gqs', q_block.astype(jnp.float32), key_block.astype(jnp.float32)) * scale
        shifted = jnp.exp(scores - lax.optimization_barrier(jnp.max(scores, axis=-1, keepdims=True)))
        weights = (shifted / lax.optimization_barrier(jnp.sum(shifted, axis=-1, keepdims=True))).astype(jnp.bfloat16)
        return jnp.einsum('gqs,sd->qgd', weights.astype(jnp.float32), value_block.astype(jnp.float32)).astype(jnp.bfloat16)
    results = lax.map(one_item, jnp.arange(blocks * kv_count, dtype=jnp.int32))
    results = results.reshape(blocks, kv_count, block, group_size, head_width).transpose(0, 2, 1, 3, 4)
    return results.reshape(count_q, kv_count * group_size * head_width)

def rms_scale(values, gain_vec):
    floats = values.astype(jnp.float32)
    return floats * lax.rsqrt(lax.optimization_barrier(jnp.mean(floats * floats, axis=-1, keepdims=True)) + EPSILON) * gain_vec

def reference(residual_in, query_proj, key_proj, value_proj, query_gain, key_gain, out_weight, post_gain, pre_gain, route_ids, group_weight, first_share, gate_weight, up_weight, down_weight):
    group_size = HEADS // KV_HEADS

    def one_sequence(inputs):
        query_seq, key_seq, value_seq = inputs
        positions = jnp.arange(SEQ, dtype=jnp.int32)
        query_turned = rotate_heads(query_seq.reshape(SEQ, HEADS, HEAD_DIM), query_gain, positions)
        key_turned = rotate_heads(key_seq.reshape(SEQ, KV_HEADS, HEAD_DIM), key_gain, positions)
        return attend_blocks(query_turned.reshape(SEQ, KV_HEADS, group_size, HEAD_DIM), key_turned, value_seq.reshape(SEQ, KV_HEADS, HEAD_DIM))
    attended = lax.map(one_sequence, (query_proj, key_proj, value_proj)).reshape(SEQS * SEQ, D)
    mixed = jnp.dot(attended, out_weight, preferred_element_type=jnp.float32).astype(jnp.bfloat16)
    stream = (residual_in.reshape(SEQS * SEQ, D).astype(jnp.float32) + rms_scale(mixed, post_gain)).astype(jnp.bfloat16)
    normed = rms_scale(stream, pre_gain).astype(jnp.bfloat16)
    chosen = route_ids.reshape(-1).astype(jnp.int32)
    assigns = chosen.shape[0]
    order = jnp.argsort(chosen, stable=True).astype(jnp.int32)
    counts = jax.ops.segment_sum(jnp.ones((assigns,), jnp.int32), chosen, num_segments=EXPERTS).astype(jnp.int32)
    starts = (jnp.cumsum(counts) - counts).astype(jnp.int32)
    most = CAP * N_SP * N_DP
    order_pad = jnp.concatenate([order, jnp.full((most,), assigns, jnp.int32)])
    normed_pad = jnp.concatenate([normed, jnp.zeros((1, D), jnp.bfloat16)], axis=0)

    def per_expert(carry, inputs):
        index, gate_one, up_one, down_one = inputs
        picked = lax.dynamic_slice(order_pad, (starts[index].astype(jnp.int32),), (most,))
        valid = jnp.arange(most, dtype=jnp.int32) < counts[index]
        picked = jnp.where(valid, picked, assigns).astype(jnp.int32)
        rows_in = normed_pad[picked // 2]
        gated = jnp.dot(rows_in, gate_one, preferred_element_type=jnp.float32)
        lifted = jnp.dot(rows_in, up_one, preferred_element_type=jnp.float32)
        hidden = (jax.nn.silu(gated) * lifted).astype(jnp.bfloat16)
        produced = jnp.dot(hidden, down_one, preferred_element_type=jnp.float32).astype(jnp.bfloat16)
        return (carry.at[picked].set(produced), None)
    outputs, _ = lax.scan(per_expert, jnp.zeros((assigns + 1, D), jnp.bfloat16), (jnp.arange(EXPERTS, dtype=jnp.int32), gate_weight, up_weight, down_weight))
    results = outputs[:assigns].astype(jnp.float32).reshape(SEQS * SEQ, 2, D)
    share = first_share.reshape(-1)
    weight_pair = group_weight.reshape(-1)[:, None] * jnp.stack([share, 1.0 - share], axis=1)
    combined = lax.optimization_barrier(jnp.sum(weight_pair[:, :, None] * results, axis=1))
    return (stream.astype(jnp.float32) + combined).astype(jnp.bfloat16).reshape(SEQS, SEQ, D)
```

```python
import functools

import jax
import jax.numpy as jnp
import numpy as np
from jax import lax
from jax.experimental import pallas as pl
from jax.experimental.pallas import tpu as pltpu
from jax.sharding import PartitionSpec as P

HEAD_DIM = 128
GRID_W = 64
GROUPS = 4
EPSILON = 1e-06
MESH = pl.DeviceIdType.MESH
VMEM_LIMIT = 60 * 1024 * 1024
F32 = jnp.float32
BF16 = jnp.bfloat16


def angle_tables(length):
    quarter = HEAD_DIM // 4
    inverse = 10000.0 ** (-np.arange(quarter, dtype=np.float64) / quarter)
    positions = np.arange(length)
    rows = (positions // GRID_W)[:, None] * inverse
    cols = (positions % GRID_W)[:, None] * inverse
    angles = np.concatenate([rows, rows, cols, cols], axis=-1)
    sign = np.where(np.arange(HEAD_DIM) % (2 * quarter) < quarter, -1.0, 1.0)
    return np.cos(angles).astype(np.float32), (np.sin(angles) * sign).astype(np.float32)


def rotate(raw, gain, cos, sin):
    floats = raw.astype(F32)
    normed = floats * lax.rsqrt(jnp.mean(floats * floats, axis=-1, keepdims=True) + EPSILON) * gain
    quarter = HEAD_DIM // 4
    lane = lax.broadcasted_iota(jnp.int32, normed.shape, 1)
    turned = jnp.where(
        (lane & (2 * quarter - 1)) < quarter,
        pltpu.roll(normed, HEAD_DIM - quarter, 1),
        pltpu.roll(normed, quarter, 1),
    )
    return (normed * cos + turned * sin).astype(BF16)


def remote(src, dst, send_sem, recv_sem, device):
    return pltpu.make_async_remote_copy(
        src_ref=src,
        dst_ref=dst,
        send_sem=send_sem,
        recv_sem=recv_sem,
        device_id=device,
        device_id_type=MESH,
    )


def attention_kernel(
    nz, nx,
    q_ref, k_ref, v_ref, qg_ref, kg_ref, cos_ref, sin_ref, res_ref, post_ref, pre_ref, ow_hbm,
    stream_ref, normed_ref,
    k_all, v_all, q_rot, k_rot, att, mixed, ow, ow_sem,
    rk, rv, skx, sku, skd, svx, svu, svd,
):
    tokens, width = q_ref.shape
    heads = width // HEAD_DIM
    kv_heads = k_ref.shape[1] // HEAD_DIM
    group = heads // kv_heads
    me = lax.axis_index("sp")
    dp = lax.axis_index("dp")
    z, x = me // nx, me % nx
    up, down = (me + nx, dp), (me - nx, dp)
    has_up, has_down = z < nz - 1, z > 0

    load_ow = pltpu.make_async_copy(ow_hbm, ow, ow_sem)
    load_ow.start()

    barrier = pltpu.get_barrier_semaphore()
    around = [(lax.rem(z + 1, nz) * nx + x, dp), (lax.rem(z + nz - 1, nz) * nx + x, dp)]
    beside = [(z * nx + lax.rem(x + off, nx), dp) for off in range(1, nx)]
    for device in around + beside:
        pl.semaphore_signal(barrier, inc=1, device_id=device, device_id_type=MESH)
    pl.semaphore_wait(barrier, len(around) + len(beside))

    def pass_on(src, buf, recv, send_up, send_down, slot, when_up, when_down):
        @pl.when(when_up)
        def _():
            remote(src, buf.at[slot], send_up.at[slot], recv.at[slot], up).start()

        @pl.when(when_down)
        def _():
            remote(src, buf.at[slot], send_down.at[slot], recv.at[slot], down).start()

    def spread(src, slot):
        for off in range(1, nx):
            remote(
                src, v_all.at[slot], svx.at[slot, off], rv.at[slot], beside[off - 1]
            ).start()

    for off in range(1, nx):
        remote(k_ref, k_all.at[me], skx.at[off], rk.at[me], beside[off - 1]).start()
    pass_on(k_ref, k_all, rk, sku, skd, me, has_up, has_down)
    pass_on(v_ref, v_all, rv, svu, svd, me, has_up, has_down)
    spread(v_ref, me)

    def arrived(buf, recv, slot):
        remote(buf.at[slot], buf.at[slot], recv.at[slot], recv.at[slot], up).wait_recv()

    def place_keys(src, slot):
        start = pl.multiple_of(slot * tokens, tokens)
        cos = cos_ref[pl.ds(start, tokens), :]
        sin = sin_ref[pl.ds(start, tokens), :]
        for head in range(kv_heads):
            k_rot[head, pl.ds(start, tokens), :] = rotate(
                src[:, head * HEAD_DIM : (head + 1) * HEAD_DIM], kg_ref[...], cos, sin
            )

    own = pl.multiple_of(me * tokens, tokens)
    q_cos = cos_ref[pl.ds(own, tokens), :]
    q_sin = sin_ref[pl.ds(own, tokens), :]
    for head in range(heads):
        q_rot[head] = rotate(
            q_ref[:, head * HEAD_DIM : (head + 1) * HEAD_DIM], qg_ref[...], q_cos, q_sin
        )
    v_all[me] = v_ref[...]

    for off in range(1, nx):
        slot = z * nx + lax.rem(x + off, nx)
        arrived(k_all, rk, slot)
        pass_on(k_all.at[slot], k_all, rk, sku, skd, slot, has_up, has_down)
    place_keys(k_ref, me)
    for off in range(1, nx):
        slot = z * nx + lax.rem(x + off, nx)
        place_keys(k_all.at[slot], slot)

    for dist in range(1, nz):
        for below in (True, False):
            source = z - dist if below else z + dist
            present = source >= 0 if below else source < nz

            @pl.when(present)
            def _(source=source, below=below):
                for off in range(nx):
                    slot = source * nx + lax.rem(x + off, nx)
                    arrived(k_all, rk, slot)
                    pass_on(
                        k_all.at[slot], k_all, rk, sku, skd, slot,
                        has_up if below else False, False if below else has_down,
                    )
                slot = source * nx + x
                arrived(v_all, rv, slot)
                pass_on(
                    v_all.at[slot], v_all, rv, svu, svd, slot,
                    has_up if below else False, False if below else has_down,
                )
                spread(v_all.at[slot], slot)
                for off in range(nx):
                    slot = source * nx + lax.rem(x + off, nx)
                    place_keys(k_all.at[slot], slot)

    for plane in range(nz):
        for off in range(1, nx):
            arrived(v_all, rv, plane * nx + lax.rem(x + off, nx))

    length = nz * nx * tokens
    factor = float(HEAD_DIM**-0.5 * np.log2(np.e))

    def one_group(kv, carry):
        lanes = pl.ds(pl.multiple_of(kv * HEAD_DIM, HEAD_DIM), HEAD_DIM)
        keys = k_rot[kv]
        values = v_all[:, :, lanes].reshape(length, HEAD_DIM)
        for member in range(group):
            head = kv * group + member
            scores = lax.dot_general(
                q_rot[head], keys, (((1,), (1,)), ((), ())), preferred_element_type=F32
            )
            top = jnp.max(scores, axis=-1, keepdims=True)
            raised = jnp.exp2((scores - top) * factor)
            probs = (raised * (1.0 / jnp.sum(raised, axis=-1, keepdims=True))).astype(BF16)
            columns = pl.ds(pl.multiple_of(head * HEAD_DIM, HEAD_DIM), HEAD_DIM)
            att[:, columns] = jnp.dot(probs, values, preferred_element_type=F32).astype(BF16)
        return carry

    lax.fori_loop(0, kv_heads, one_group, 0)

    load_ow.wait()
    tile = 512

    def one_tile(step, carry):
        columns = pl.ds(pl.multiple_of(step * tile, tile), tile)
        mixed[:, columns] = jnp.dot(
            att[...], ow[:, columns], preferred_element_type=F32
        ).astype(BF16)
        return carry

    lax.fori_loop(0, width // tile, one_tile, 0)

    blend = mixed[...].astype(F32)
    blend = blend * lax.rsqrt(jnp.mean(blend * blend, axis=-1, keepdims=True) + EPSILON)
    stream = (res_ref[...].astype(F32) + blend * post_ref[...]).astype(BF16)
    stream_ref[...] = stream
    wide = stream.astype(F32)
    wide = wide * lax.rsqrt(jnp.mean(wide * wide, axis=-1, keepdims=True) + EPSILON)
    normed_ref[...] = (wide * pre_ref[...]).astype(BF16)

    def sent(src, sem, device):
        remote(src, src, sem, sem, device).wait_send()

    for off in range(1, nx):
        sent(k_ref, skx.at[off], beside[off - 1])
    for plane in range(nz):
        for off in range(nx):
            slot = plane * nx + lax.rem(x + off, nx)

            @pl.when(jnp.logical_and(has_up, z >= plane))
            def _(slot=slot, off=off):
                sent(k_all.at[slot], sku.at[slot], up)
                if off == 0:
                    sent(v_all.at[slot], svu.at[slot], up)

            @pl.when(jnp.logical_and(has_down, z <= plane))
            def _(slot=slot, off=off):
                sent(k_all.at[slot], skd.at[slot], down)
                if off == 0:
                    sent(v_all.at[slot], svd.at[slot], down)

        slot = plane * nx + x
        for off in range(1, nx):
            sent(v_all.at[slot], svx.at[slot, off], beside[off - 1])


def before(tokens):
    row = lax.broadcasted_iota(jnp.int32, (tokens, tokens), 0)
    col = lax.broadcasted_iota(jnp.int32, (tokens, tokens), 1)
    return (row < col).astype(F32).astype(BF16)


def group_choice(meta, first_expert, count, rows):
    tokens = meta.shape[1]
    low = first_expert.astype(F32)
    member = jnp.where((meta[0:1] >= low) & (meta[0:1] < low + float(count)), 1.0, 0.0)
    rank = jnp.dot(
        jnp.broadcast_to(member, (8, tokens)).astype(BF16),
        before(tokens),
        preferred_element_type=F32,
    )[0:1]
    place = lax.broadcasted_iota(jnp.int32, (rows, tokens), 0).astype(F32)
    return jnp.where(rank == place, 1.0, 0.0) * member


def slot_choice(meta, first_expert, count, cap):
    tokens = meta.shape[1]
    names = lax.broadcasted_iota(jnp.int32, (count, tokens), 0).astype(F32)
    names = names + first_expert.astype(F32)
    first = jnp.where(meta[0:1] == names, 1.0, 0.0)
    second = jnp.where(meta[1:2] == names, 1.0, 0.0)
    rank = jnp.dot((first + second).astype(BF16), before(tokens), preferred_element_type=F32)
    row = lax.broadcasted_iota(jnp.int32, (count * cap, count), 0)
    start = lax.broadcasted_iota(jnp.int32, (count * cap, count), 1) * cap
    widen = jnp.where((row >= start) & (row < start + cap), 1.0, 0.0).astype(BF16)

    def widened(values):
        return jnp.dot(widen, values.astype(BF16), preferred_element_type=F32)

    place = lax.broadcasted_iota(jnp.int32, (count * cap, tokens), 0) & (cap - 1)
    hit = jnp.where(widened(rank) == place.astype(F32), 1.0, 0.0)
    return widened(first) * hit, widened(second) * hit


def contract(left, right, dims):
    return lax.dot_general(
        left.astype(BF16), right.astype(BF16), ((dims[:1], dims[1:]), ((), ())),
        preferred_element_type=F32,
    )


def expert_kernel(
    nz, nx, n_dp,
    normed_ref, stream_ref, meta_ref, wg_hbm, wu_hbm, wd_hbm,
    out_ref,
    wg, wu, wd, w_sem, p1, r1, metas, p2, r2, o2, back, mix, fin,
    s1, t1, sm, tm, s2, t2, s3, t3, s4, t4,
):
    tokens, width = normed_ref.shape
    count, cap = p2.shape[1], p2.shape[2]
    rows = p1.shape[1]
    sp = lax.axis_index("sp")
    dp = lax.axis_index("dp")
    z, x = sp // nx, sp % nx
    me = x * n_dp + dp

    loads = [
        pltpu.make_async_copy(src, dst, w_sem.at[i])
        for i, (src, dst) in enumerate(((wg_hbm, wg), (wu_hbm, wu), (wd_hbm, wd)))
    ]
    for load in loads:
        load.start()

    def plane_peer(off):
        j = lax.rem(me + off, count)
        return j, (z * nx + j // n_dp, j % n_dp)

    def column_peer(dist):
        plane = lax.rem(z + dist, nz)
        return plane, (plane * nx + x, dp)

    barrier = pltpu.get_barrier_semaphore()
    for off in range(1, count):
        pl.semaphore_signal(barrier, inc=1, device_id=plane_peer(off)[1], device_id_type=MESH)
    for dist in range(1, nz):
        pl.semaphore_signal(barrier, inc=1, device_id=column_peer(dist)[1], device_id_type=MESH)

    meta = meta_ref[...]
    for g in range(nz):
        pick = group_choice(meta, jnp.int32(g * count), count, rows)
        p1[g] = contract(pick, normed_ref[...], (1, 0)).astype(BF16)
    metas[z] = meta
    r1[z] = p1[z]

    pl.semaphore_wait(barrier, count - 1 + nz - 1)
    for dist in range(1, nz):
        plane, device = column_peer(dist)
        remote(meta_ref, metas.at[z], sm.at[plane], tm.at[z], device).start()
        remote(p1.at[plane], r1.at[z], s1.at[plane], t1.at[z], device).start()

    first_expert = z * count

    def dispatch(dist, carry):
        source, device = column_peer(dist)

        @pl.when(dist > 0)
        def _():
            remote(meta_ref, metas.at[source], sm.at[source], tm.at[source], device).wait_recv()
            remote(p1.at[source], r1.at[source], s1.at[source], t1.at[source], device).wait_recv()

        got = metas[source]
        group = group_choice(got, first_expert, count, rows)
        first, second = slot_choice(got, first_expert, count, cap)
        pick = contract(first + second, group, (1, 1))
        packed = contract(pick, r1[source], (1, 0)).astype(BF16)
        p2[source] = packed.reshape(count, cap, width)
        r2[source, me] = p2[source, me]
        for off in range(1, count):
            j, device = plane_peer(off)
            remote(
                p2.at[source, j], r2.at[source, me], s2.at[source, j], t2.at[source, me], device
            ).start()
        return carry

    lax.fori_loop(0, nz, dispatch, 0)
    for load in loads:
        load.wait()

    def transform(dist, carry):
        source = lax.rem(z + dist, nz)
        for off in range(1, count):
            j, device = plane_peer(off)
            remote(
                p2.at[source, j], r2.at[source, j], s2.at[source, j], t2.at[source, j], device
            ).wait_recv()
        arrived = r2[source].reshape(count * cap, width)
        gated = jnp.dot(arrived, wg[...], preferred_element_type=F32)
        lifted = jnp.dot(arrived, wu[...], preferred_element_type=F32)
        hidden = (gated / (1.0 + jnp.exp(-gated)) * lifted).astype(BF16)
        result = jnp.dot(hidden, wd[...], preferred_element_type=F32).astype(BF16)
        o2[source] = result.reshape(count, cap, width)
        back[source, me] = o2[source, me]
        for off in range(1, count):
            j, device = plane_peer(off)
            remote(
                o2.at[source, j], back.at[source, me], s3.at[source, j], t3.at[source, me], device
            ).start()
        return carry

    lax.fori_loop(0, nz, transform, 0)

    def combine(dist, carry):
        source, column = column_peer(dist)
        for off in range(1, count):
            j, device = plane_peer(off)
            remote(
                o2.at[source, j], back.at[source, j], s3.at[source, j], t3.at[source, j], device
            ).wait_recv()
        got = metas[source]
        group = group_choice(got, first_expert, count, rows)
        first, second = slot_choice(got, first_expert, count, cap)
        outs = back[source].reshape(count * cap, width)
        one = contract(contract(group, first, (1, 1)), outs, (1, 0))
        two = contract(contract(group, second, (1, 1)), outs, (1, 0))
        weight = jnp.sum(group * got[2:3], axis=1, keepdims=True)
        share = jnp.sum(group * got[3:4], axis=1, keepdims=True)
        total = (weight * (share * one + (1.0 - share) * two)).astype(BF16)
        mix[source] = total

        @pl.when(dist == 0)
        def _():
            fin[source] = total

        @pl.when(dist > 0)
        def _():
            remote(mix.at[source], fin.at[z], s4.at[source], t4.at[z], column).start()

        return carry

    lax.fori_loop(0, nz, combine, 0)

    picks = [
        group_choice(meta, jnp.int32(g * count), count, rows) for g in range(nz)
    ]
    for dist in range(1, nz):
        plane, device = column_peer(dist)
        remote(mix.at[plane], fin.at[plane], s4.at[plane], t4.at[plane], device).wait_recv()
    every = jnp.concatenate(picks, axis=0)
    added = contract(every, fin[...].reshape(tokens, width), (0, 0))
    out_ref[...] = (stream_ref[...].astype(F32) + added).astype(BF16)

    for dist in range(1, nz):
        plane, device = column_peer(dist)
        remote(meta_ref, metas.at[z], sm.at[plane], tm.at[z], device).wait_send()
        remote(p1.at[plane], r1.at[z], s1.at[plane], t1.at[z], device).wait_send()
        remote(mix.at[plane], fin.at[z], s4.at[plane], t4.at[z], device).wait_send()

    def drain(source, carry):
        for off in range(1, count):
            j, device = plane_peer(off)
            remote(
                p2.at[source, j], r2.at[source, me], s2.at[source, j], t2.at[source, me], device
            ).wait_send()
            remote(
                o2.at[source, j], back.at[source, me], s3.at[source, j], t3.at[source, me], device
            ).wait_send()
        return carry

    lax.fori_loop(0, nz, drain, 0)


def local(
    residual_in, query_proj, key_proj, value_proj, query_gain, key_gain, out_weight, post_gain,
    pre_gain, route_ids, group_weight, first_share, gate_weight, up_weight, down_weight,
):
    n_sp = lax.axis_size("sp")
    n_dp = lax.axis_size("dp")
    tokens, width = query_proj.shape[1:]
    kv_width = key_proj.shape[2]
    heads, kv_heads = width // HEAD_DIM, kv_width // HEAD_DIM
    nz = GROUPS
    nx = n_sp // nz
    length = n_sp * tokens
    cos, sin = angle_tables(length)
    vmem = pl.BlockSpec(memory_space=pltpu.VMEM)
    hbm = pl.BlockSpec(memory_space=pl.ANY)
    dma = pltpu.SemaphoreType.DMA
    row = jax.ShapeDtypeStruct((tokens, width), BF16)
    stream, normed = pl.pallas_call(
        functools.partial(attention_kernel, nz, nx),
        out_shape=(row, row),
        in_specs=[vmem] * 10 + [hbm],
        out_specs=(vmem, vmem),
        scratch_shapes=[
            pltpu.VMEM((n_sp, tokens, kv_width), BF16),
            pltpu.VMEM((n_sp, tokens, kv_width), BF16),
            pltpu.VMEM((heads, tokens, HEAD_DIM), BF16),
            pltpu.VMEM((kv_heads, length, HEAD_DIM), BF16),
            pltpu.VMEM((tokens, width), BF16),
            pltpu.VMEM((tokens, width), BF16),
            pltpu.VMEM((width, width), BF16),
            dma,
            dma((n_sp,)), dma((n_sp,)),
            dma((nx,)), dma((n_sp,)), dma((n_sp,)),
            dma((n_sp, nx)), dma((n_sp,)), dma((n_sp,)),
        ],
        compiler_params=pltpu.CompilerParams(
            collective_id=0, has_side_effects=True, vmem_limit_bytes=VMEM_LIMIT
        ),
        name="attention",
    )(
        query_proj[0], key_proj[0], value_proj[0],
        query_gain.reshape(1, -1), key_gain.reshape(1, -1),
        jnp.asarray(cos), jnp.asarray(sin),
        residual_in[0], post_gain.reshape(1, -1), pre_gain.reshape(1, -1), out_weight,
    )

    experts = gate_weight.shape[0] * n_sp * n_dp
    count = experts // nz
    cap = max(16, 4 * tokens // experts)
    rows = tokens // nz
    ff = gate_weight.shape[2]
    meta = jnp.concatenate(
        [route_ids[0].T.astype(F32), group_weight, first_share, jnp.zeros((4, tokens), F32)], axis=0
    )
    blocks = pltpu.VMEM((nz, count, cap, width), BF16)
    lines = pltpu.VMEM((nz, rows, width), BF16)
    out = pl.pallas_call(
        functools.partial(expert_kernel, nz, nx, n_dp),
        out_shape=row,
        in_specs=[vmem] * 3 + [hbm] * 3,
        out_specs=vmem,
        scratch_shapes=[
            pltpu.VMEM((width, ff), BF16),
            pltpu.VMEM((width, ff), BF16),
            pltpu.VMEM((ff, width), BF16),
            dma((3,)),
            lines, lines,
            pltpu.VMEM((nz, 8, tokens), F32),
            blocks, blocks, blocks, blocks,
            lines, lines,
            dma((nz,)), dma((nz,)), dma((nz,)), dma((nz,)),
            dma((nz, count)), dma((nz, count)), dma((nz, count)), dma((nz, count)),
            dma((nz,)), dma((nz,)),
        ],
        compiler_params=pltpu.CompilerParams(
            collective_id=1, has_side_effects=True, vmem_limit_bytes=VMEM_LIMIT
        ),
        name="experts",
    )(normed, stream, meta, gate_weight[0], up_weight[0], down_weight[0])
    return out.reshape(1, tokens, width)


def solution(mesh):
    tok3 = P("dp", "sp", None)
    tok2 = P("dp", "sp")
    weight = P(("sp", "dp"), None, None)
    placed = (
        tok3, tok3, tok3, tok3, P(), P(), P(), P(), P(), tok3, tok2, tok2, weight, weight, weight,
    )
    return jax.shard_map(
        local, mesh=mesh, in_specs=placed, out_specs=P("dp", "sp", None), check_vma=False
    )
```

```python
import functools

import jax
import jax.numpy as jnp
import numpy as np
from jax import lax
from jax.experimental import pallas as pl
from jax.experimental.pallas import tpu as pltpu
from jax.sharding import PartitionSpec as P

HEAD_DIM = 128
GRID_W = 64
GROUPS = 4
EPSILON = 1e-06
MESH = pl.DeviceIdType.MESH
VMEM_LIMIT = 60 * 1024 * 1024
F32 = jnp.float32
BF16 = jnp.bfloat16


def angle_tables(length):
    quarter = HEAD_DIM // 4
    inverse = 10000.0 ** (-np.arange(quarter, dtype=np.float64) / quarter)
    positions = np.arange(length)
    rows = (positions // GRID_W)[:, None] * inverse
    cols = (positions % GRID_W)[:, None] * inverse
    angles = np.concatenate([rows, rows, cols, cols], axis=-1)
    sign = np.where(np.arange(HEAD_DIM) % (2 * quarter) < quarter, -1.0, 1.0)
    return np.cos(angles).astype(np.float32), (np.sin(angles) * sign).astype(np.float32)


def rotate(raw, gain, cos, sin):
    floats = raw.astype(F32)
    normed = floats * lax.rsqrt(jnp.mean(floats * floats, axis=-1, keepdims=True) + EPSILON) * gain
    quarter = HEAD_DIM // 4
    lane = lax.broadcasted_iota(jnp.int32, normed.shape, 1)
    turned = jnp.where(
        (lane & (2 * quarter - 1)) < quarter,
        pltpu.roll(normed, HEAD_DIM - quarter, 1),
        pltpu.roll(normed, quarter, 1),
    )
    return (normed * cos + turned * sin).astype(BF16)


def remote(src, dst, send_sem, recv_sem, device):
    return pltpu.make_async_remote_copy(
        src_ref=src,
        dst_ref=dst,
        send_sem=send_sem,
        recv_sem=recv_sem,
        device_id=device,
        device_id_type=MESH,
    )


def attention_kernel(
    nz, nx,
    q_ref, k_ref, v_ref, qg_ref, kg_ref, cos_ref, sin_ref, res_ref, post_ref, pre_ref, ow_hbm,
    stream_ref, normed_ref,
    k_all, v_all, q_rot, k_rot, att, acc, ow, ow_sem,
    rk, rv, skx, sku, skd, svx, svu, svd,
):
    tokens, width = q_ref.shape
    heads = width // HEAD_DIM
    kv_heads = k_ref.shape[1] // HEAD_DIM
    group = heads // kv_heads
    me = lax.axis_index("sp")
    dp = lax.axis_index("dp")
    z, x = me // nx, me % nx
    up, down = (me + nx, dp), (me - nx, dp)
    has_up, has_down = z < nz - 1, z > 0
    both = ((k_ref, k_all, rk, skx, sku, skd), (v_ref, v_all, rv, svx, svu, svd))

    load_ow = pltpu.make_async_copy(ow_hbm, ow, ow_sem)
    load_ow.start()

    barrier = pltpu.get_barrier_semaphore()
    around = [(lax.rem(z + 1, nz) * nx + x, dp), (lax.rem(z + nz - 1, nz) * nx + x, dp)]
    beside = [(z * nx + lax.rem(x + off, nx), dp) for off in range(1, nx)]
    for device in around + beside:
        pl.semaphore_signal(barrier, inc=1, device_id=device, device_id_type=MESH)
    pl.semaphore_wait(barrier, len(around) + len(beside))

    def lanes_of(head):
        return pl.ds(pl.multiple_of(head * HEAD_DIM, HEAD_DIM), HEAD_DIM)

    def hop(src, buf, recv, send, slot, head, device):
        return remote(src, buf.at[slot, head], send, recv.at[slot, head], device)

    def send_own(head):
        for raw, buf, recv, sx, su, sd in both:
            src = raw.at[:, lanes_of(head)]

            @pl.when(has_up)
            def _():
                hop(src, buf, recv, su.at[me, head], me, head, up).start()

            @pl.when(has_down)
            def _():
                hop(src, buf, recv, sd.at[me, head], me, head, down).start()

        for raw, buf, recv, sx, su, sd in both:
            src = raw.at[:, lanes_of(head)]
            for off in range(1, nx):
                hop(src, buf, recv, sx.at[me, head, off], me, head, beside[off - 1]).start()

    def arrived(buf, recv, slot, head):
        block = buf.at[slot, head]
        remote(block, block, recv.at[slot, head], recv.at[slot, head], up).wait_recv()

    def relay(head):
        for dist in range(1, nz):
            for below in (True, False):
                source = z - dist if below else z + dist
                present = source >= 0 if below else source < nz
                further = has_up if below else has_down
                onward = up if below else down

                @pl.when(present)
                def _(source=source, below=below, further=further, onward=onward):
                    slot = source * nx + x
                    for _raw, buf, recv, sx, su, sd in both:
                        arrived(buf, recv, slot, head)
                        src = buf.at[slot, head]
                        send = su if below else sd

                        @pl.when(further)
                        def _(src=src, buf=buf, recv=recv, send=send):
                            hop(src, buf, recv, send.at[slot, head], slot, head, onward).start()

                        for off in range(1, nx):
                            hop(
                                src, buf, recv, sx.at[slot, head, off], slot, head,
                                beside[off - 1],
                            ).start()

    length = nz * nx * tokens
    factor = float(HEAD_DIM**-0.5 * np.log2(np.e))
    span = group * HEAD_DIM

    def attend(kv):
        for plane in range(nz):
            for off in range(1, nx):
                slot = plane * nx + lax.rem(x + off, nx)
                arrived(k_all, rk, slot, kv)
                arrived(v_all, rv, slot, kv)
        k_all[me, kv] = k_ref[:, lanes_of(kv)]
        v_all[me, kv] = v_ref[:, lanes_of(kv)]

        def place(slot, carry):
            rows = pl.ds(pl.multiple_of(slot * tokens, tokens), tokens)
            k_rot[rows, :] = rotate(k_all[slot, kv], kg_ref[...], cos_ref[rows, :], sin_ref[rows, :])
            return carry

        lax.fori_loop(0, nz * nx, place, 0)
        keys = k_rot[...]
        values = v_all[:, kv].reshape(length, HEAD_DIM)
        for member in range(group):
            scores = lax.dot_general(
                q_rot[kv * group + member], keys, (((1,), (1,)), ((), ())),
                preferred_element_type=F32,
            )
            top = jnp.max(scores, axis=-1, keepdims=True)
            raised = jnp.exp2((scores - top) * factor)
            probs = (raised * (1.0 / jnp.sum(raised, axis=-1, keepdims=True))).astype(BF16)
            att[:, member * HEAD_DIM : (member + 1) * HEAD_DIM] = jnp.dot(
                probs, values, preferred_element_type=F32
            ).astype(BF16)
        part = ow.at[pl.ds(pl.multiple_of(kv * span, span), span), :]
        tile = 1024
        for start in range(0, width, tile):
            columns = slice(start, start + tile)
            acc[:, columns] += jnp.dot(att[...], part[:, columns], preferred_element_type=F32)

    send_own(0)
    for head in range(1, min(3, kv_heads)):
        send_own(head)
    own = pl.multiple_of(me * tokens, tokens)
    q_cos = cos_ref[pl.ds(own, tokens), :]
    q_sin = sin_ref[pl.ds(own, tokens), :]
    for head in range(heads):
        q_rot[head] = rotate(
            q_ref[:, head * HEAD_DIM : (head + 1) * HEAD_DIM], qg_ref[...], q_cos, q_sin
        )
    acc[...] = jnp.zeros_like(acc)
    relay(0)
    load_ow.wait()

    def one_head(kv, carry):
        @pl.when(kv + 3 < kv_heads)
        def _():
            send_own(kv + 3)

        @pl.when(kv + 1 < kv_heads)
        def _():
            relay(kv + 1)

        attend(kv)
        return carry

    lax.fori_loop(0, kv_heads, one_head, 0)

    blend = acc[...].astype(BF16).astype(F32)
    blend = blend * lax.rsqrt(jnp.mean(blend * blend, axis=-1, keepdims=True) + EPSILON)
    stream = (res_ref[...].astype(F32) + blend * post_ref[...]).astype(BF16)
    stream_ref[...] = stream
    wide = stream.astype(F32)
    wide = wide * lax.rsqrt(jnp.mean(wide * wide, axis=-1, keepdims=True) + EPSILON)
    normed_ref[...] = (wide * pre_ref[...]).astype(BF16)

    def sent(buf, sem, device):
        block = buf.at[0, 0]
        remote(block, block, sem, sem, device).wait_send()

    def drain(head, carry):
        for _raw, buf, recv, sx, su, sd in both:
            for plane in range(nz):
                slot = plane * nx + x

                @pl.when(jnp.logical_and(has_up, z >= plane))
                def _(slot=slot):
                    sent(buf, su.at[slot, head], up)

                @pl.when(jnp.logical_and(has_down, z <= plane))
                def _(slot=slot):
                    sent(buf, sd.at[slot, head], down)

                for off in range(1, nx):
                    sent(buf, sx.at[slot, head, off], beside[off - 1])
        return carry

    lax.fori_loop(0, kv_heads, drain, 0)


def before(tokens):
    row = lax.broadcasted_iota(jnp.int32, (tokens, tokens), 0)
    col = lax.broadcasted_iota(jnp.int32, (tokens, tokens), 1)
    return (row < col).astype(F32).astype(BF16)


def group_choice(meta, first_expert, count, rows):
    tokens = meta.shape[1]
    low = first_expert.astype(F32)
    member = jnp.where((meta[0:1] >= low) & (meta[0:1] < low + float(count)), 1.0, 0.0)
    rank = jnp.dot(
        jnp.broadcast_to(member, (8, tokens)).astype(BF16),
        before(tokens),
        preferred_element_type=F32,
    )[0:1]
    place = lax.broadcasted_iota(jnp.int32, (rows, tokens), 0).astype(F32)
    return jnp.where(rank == place, 1.0, 0.0) * member


def slot_choice(meta, first_expert, count, cap):
    tokens = meta.shape[1]
    names = lax.broadcasted_iota(jnp.int32, (count, tokens), 0).astype(F32)
    names = names + first_expert.astype(F32)
    first = jnp.where(meta[0:1] == names, 1.0, 0.0)
    second = jnp.where(meta[1:2] == names, 1.0, 0.0)
    rank = jnp.dot((first + second).astype(BF16), before(tokens), preferred_element_type=F32)
    row = lax.broadcasted_iota(jnp.int32, (count * cap, count), 0)
    start = lax.broadcasted_iota(jnp.int32, (count * cap, count), 1) * cap
    widen = jnp.where((row >= start) & (row < start + cap), 1.0, 0.0).astype(BF16)

    def widened(values):
        return jnp.dot(widen, values.astype(BF16), preferred_element_type=F32)

    place = lax.broadcasted_iota(jnp.int32, (count * cap, tokens), 0) & (cap - 1)
    hit = jnp.where(widened(rank) == place.astype(F32), 1.0, 0.0)
    return widened(first) * hit, widened(second) * hit


def contract(left, right, dims):
    return lax.dot_general(
        left.astype(BF16), right.astype(BF16), ((dims[:1], dims[1:]), ((), ())),
        preferred_element_type=F32,
    )


def expert_kernel(
    nz, nx, n_dp,
    normed_ref, stream_ref, meta_ref, wg_hbm, wu_hbm, wd_hbm,
    out_ref,
    wg, wu, wd, w_sem, p1, r1, metas, p2, r2, o2, back, mix, fin,
    s1, t1, sm, tm, s2, t2, s3, t3, s4, t4,
):
    tokens, width = normed_ref.shape
    count, cap = p2.shape[1], p2.shape[2]
    rows = p1.shape[1]
    sp = lax.axis_index("sp")
    dp = lax.axis_index("dp")
    z, x = sp // nx, sp % nx
    me = x * n_dp + dp

    loads = [
        pltpu.make_async_copy(src, dst, w_sem.at[i])
        for i, (src, dst) in enumerate(((wg_hbm, wg), (wu_hbm, wu), (wd_hbm, wd)))
    ]
    for load in loads:
        load.start()

    def plane_peer(off):
        j = lax.rem(me + off, count)
        return j, (z * nx + j // n_dp, j % n_dp)

    def column_peer(dist):
        plane = lax.rem(z + dist, nz)
        return plane, (plane * nx + x, dp)

    barrier = pltpu.get_barrier_semaphore()
    for off in range(1, count):
        pl.semaphore_signal(barrier, inc=1, device_id=plane_peer(off)[1], device_id_type=MESH)
    for dist in range(1, nz):
        pl.semaphore_signal(barrier, inc=1, device_id=column_peer(dist)[1], device_id_type=MESH)

    meta = meta_ref[...]
    for g in range(nz):
        pick = group_choice(meta, jnp.int32(g * count), count, rows)
        p1[g] = contract(pick, normed_ref[...], (1, 0)).astype(BF16)
    metas[z] = meta
    r1[z] = p1[z]

    pl.semaphore_wait(barrier, count - 1 + nz - 1)
    for dist in range(1, nz):
        plane, device = column_peer(dist)
        remote(meta_ref, metas.at[z], sm.at[plane], tm.at[z], device).start()
        remote(p1.at[plane], r1.at[z], s1.at[plane], t1.at[z], device).start()

    first_expert = z * count

    def dispatch(dist, carry):
        source, device = column_peer(dist)

        @pl.when(dist > 0)
        def _():
            remote(meta_ref, metas.at[source], sm.at[source], tm.at[source], device).wait_recv()
            remote(p1.at[source], r1.at[source], s1.at[source], t1.at[source], device).wait_recv()

        got = metas[source]
        group = group_choice(got, first_expert, count, rows)
        first, second = slot_choice(got, first_expert, count, cap)
        pick = contract(first + second, group, (1, 1))
        packed = contract(pick, r1[source], (1, 0)).astype(BF16)
        p2[source] = packed.reshape(count, cap, width)
        r2[source, me] = p2[source, me]
        for off in range(1, count):
            j, device = plane_peer(off)
            remote(
                p2.at[source, j], r2.at[source, me], s2.at[source, j], t2.at[source, me], device
            ).start()
        return carry

    lax.fori_loop(0, nz, dispatch, 0)
    for load in loads:
        load.wait()

    def transform(dist, carry):
        source = lax.rem(z + dist + 1, nz)
        for off in range(1, count):
            j, device = plane_peer(off)
            remote(
                p2.at[source, j], r2.at[source, j], s2.at[source, j], t2.at[source, j], device
            ).wait_recv()
        arrived = r2[source].reshape(count * cap, width)
        gated = jnp.dot(arrived, wg[...], preferred_element_type=F32)
        lifted = jnp.dot(arrived, wu[...], preferred_element_type=F32)
        hidden = (gated / (1.0 + jnp.exp(-gated)) * lifted).astype(BF16)
        result = jnp.dot(hidden, wd[...], preferred_element_type=F32).astype(BF16)
        o2[source] = result.reshape(count, cap, width)
        back[source, me] = o2[source, me]
        for off in range(1, count):
            j, device = plane_peer(off)
            remote(
                o2.at[source, j], back.at[source, me], s3.at[source, j], t3.at[source, me], device
            ).start()
        return carry

    lax.fori_loop(0, nz, transform, 0)

    def combine(dist, carry):
        source, column = column_peer(dist + 1)
        for off in range(1, count):
            j, device = plane_peer(off)
            remote(
                o2.at[source, j], back.at[source, j], s3.at[source, j], t3.at[source, j], device
            ).wait_recv()
        got = metas[source]
        group = group_choice(got, first_expert, count, rows)
        first, second = slot_choice(got, first_expert, count, cap)
        outs = back[source].reshape(count * cap, width)
        one = contract(contract(group, first, (1, 1)), outs, (1, 0))
        two = contract(contract(group, second, (1, 1)), outs, (1, 0))
        weight = jnp.sum(group * got[2:3], axis=1, keepdims=True)
        share = jnp.sum(group * got[3:4], axis=1, keepdims=True)
        total = (weight * (share * one + (1.0 - share) * two)).astype(BF16)
        mix[source] = total

        @pl.when(dist == nz - 1)
        def _():
            fin[source] = total

        @pl.when(dist < nz - 1)
        def _():
            remote(mix.at[source], fin.at[z], s4.at[source], t4.at[z], column).start()

        return carry

    lax.fori_loop(0, nz, combine, 0)

    picks = [
        group_choice(meta, jnp.int32(g * count), count, rows) for g in range(nz)
    ]
    for dist in range(1, nz):
        plane, device = column_peer(dist)
        remote(mix.at[plane], fin.at[plane], s4.at[plane], t4.at[plane], device).wait_recv()
    every = jnp.concatenate(picks, axis=0)
    added = contract(every, fin[...].reshape(tokens, width), (0, 0))
    out_ref[...] = (stream_ref[...].astype(F32) + added).astype(BF16)

    for dist in range(1, nz):
        plane, device = column_peer(dist)
        remote(meta_ref, metas.at[z], sm.at[plane], tm.at[z], device).wait_send()
        remote(p1.at[plane], r1.at[z], s1.at[plane], t1.at[z], device).wait_send()
        remote(mix.at[plane], fin.at[z], s4.at[plane], t4.at[z], device).wait_send()

    def drain(source, carry):
        for off in range(1, count):
            j, device = plane_peer(off)
            remote(
                p2.at[source, j], r2.at[source, me], s2.at[source, j], t2.at[source, me], device
            ).wait_send()
            remote(
                o2.at[source, j], back.at[source, me], s3.at[source, j], t3.at[source, me], device
            ).wait_send()
        return carry

    lax.fori_loop(0, nz, drain, 0)


def local(
    residual_in, query_proj, key_proj, value_proj, query_gain, key_gain, out_weight, post_gain,
    pre_gain, route_ids, group_weight, first_share, gate_weight, up_weight, down_weight,
):
    n_sp = lax.axis_size("sp")
    n_dp = lax.axis_size("dp")
    tokens, width = query_proj.shape[1:]
    kv_width = key_proj.shape[2]
    heads, kv_heads = width // HEAD_DIM, kv_width // HEAD_DIM
    nz = GROUPS
    nx = n_sp // nz
    length = n_sp * tokens
    cos, sin = angle_tables(length)
    vmem = pl.BlockSpec(memory_space=pltpu.VMEM)
    hbm = pl.BlockSpec(memory_space=pl.ANY)
    dma = pltpu.SemaphoreType.DMA
    row = jax.ShapeDtypeStruct((tokens, width), BF16)
    stream, normed = pl.pallas_call(
        functools.partial(attention_kernel, nz, nx),
        out_shape=(row, row),
        in_specs=[vmem] * 10 + [hbm],
        out_specs=(vmem, vmem),
        scratch_shapes=[
            pltpu.VMEM((n_sp, kv_heads, tokens, HEAD_DIM), BF16),
            pltpu.VMEM((n_sp, kv_heads, tokens, HEAD_DIM), BF16),
            pltpu.VMEM((heads, tokens, HEAD_DIM), BF16),
            pltpu.VMEM((length, HEAD_DIM), BF16),
            pltpu.VMEM((tokens, width // kv_heads), BF16),
            pltpu.VMEM((tokens, width), F32),
            pltpu.VMEM((width, width), BF16),
            dma,
            dma((n_sp, kv_heads)), dma((n_sp, kv_heads)),
            dma((n_sp, kv_heads, nx)), dma((n_sp, kv_heads)), dma((n_sp, kv_heads)),
            dma((n_sp, kv_heads, nx)), dma((n_sp, kv_heads)), dma((n_sp, kv_heads)),
        ],
        compiler_params=pltpu.CompilerParams(
            collective_id=0, has_side_effects=True, vmem_limit_bytes=VMEM_LIMIT
        ),
        name="attention",
    )(
        query_proj[0], key_proj[0], value_proj[0],
        query_gain.reshape(1, -1), key_gain.reshape(1, -1),
        jnp.asarray(cos), jnp.asarray(sin),
        residual_in[0], post_gain.reshape(1, -1), pre_gain.reshape(1, -1), out_weight,
    )

    experts = gate_weight.shape[0] * n_sp * n_dp
    count = experts // nz
    cap = max(16, 4 * tokens // experts)
    rows = tokens // nz
    ff = gate_weight.shape[2]
    meta = jnp.concatenate(
        [route_ids[0].T.astype(F32), group_weight, first_share, jnp.zeros((4, tokens), F32)], axis=0
    )
    blocks = pltpu.VMEM((nz, count, cap, width), BF16)
    lines = pltpu.VMEM((nz, rows, width), BF16)
    out = pl.pallas_call(
        functools.partial(expert_kernel, nz, nx, n_dp),
        out_shape=row,
        in_specs=[vmem] * 3 + [hbm] * 3,
        out_specs=vmem,
        scratch_shapes=[
            pltpu.VMEM((width, ff), BF16),
            pltpu.VMEM((width, ff), BF16),
            pltpu.VMEM((ff, width), BF16),
            dma((3,)),
            lines, lines,
            pltpu.VMEM((nz, 8, tokens), F32),
            blocks, blocks, blocks, blocks,
            lines, lines,
            dma((nz,)), dma((nz,)), dma((nz,)), dma((nz,)),
            dma((nz, count)), dma((nz, count)), dma((nz, count)), dma((nz, count)),
            dma((nz,)), dma((nz,)),
        ],
        compiler_params=pltpu.CompilerParams(
            collective_id=1, has_side_effects=True, vmem_limit_bytes=VMEM_LIMIT
        ),
        name="experts",
    )(normed, stream, meta, gate_weight[0], up_weight[0], down_weight[0])
    return out.reshape(1, tokens, width)


def solution(mesh):
    tok3 = P("dp", "sp", None)
    tok2 = P("dp", "sp")
    weight = P(("sp", "dp"), None, None)
    placed = (
        tok3, tok3, tok3, tok3, P(), P(), P(), P(), P(), tok3, tok2, tok2, weight, weight, weight,
    )
    return jax.shard_map(
        local, mesh=mesh, in_specs=placed, out_specs=P("dp", "sp", None), check_vma=False
    )
```
